32 devices in a mesh: ra: 8 (over z, y), cb: 4 (over x, core).
Axes of the slice: x: 2, y: 2, z: 4, core: 2. Of those that a mesh axis runs over, the one named last changes fastest.
Arguments:
- stream: bfloat16 [64, 1024], P(None, 'ra'), may hold values from -24 to 24, as said below
- gain_first: float32 [1024], P('ra'), may hold values from 0.5 to 1.5
- up_first: float32 [1024, 4096], P('ra', 'cb'), may hold values from -0.1875 to 0.1875
- down_first: float32 [4096, 1024], P('cb', 'ra'), may hold values from -0.09375 to 0.09375
- gain_second: float32 [1024], P('ra'), may hold values from 0.5 to 1.5
- up_second: float32 [1024, 4096], P('ra', 'cb'), may hold values from -0.1875 to 0.1875
- down_second: float32 [4096, 1024], P('cb', 'ra'), may hold values from -0.09375 to 0.09375
Outputs:
- read: bfloat16 [64, 1024], P(None, 'ra')
The draws below stay inside these ranges and needn't reach their ends.
Inputs may be any that keep to these rules, and one draw needn't show every extreme that they name: stream is of order one, and in each token one aligned block of 128 features is four times larger than the rest.
All inputs are finite; a program needn't handle non-finite values.
Results may differ from the reference program's by a relative error of at most 0.025.
Values may be sent and summed in bfloat16 or wider, within the bound.
A program may use at most 64 MiB of HBM per device.

```python
import jax
import jax.numpy as jnp
from jax import lax

D = 1024
FF = 4096
TOKENS = 64
COLS_RA = 128


def draw_stream(key, part):
    key_base, key_block = jax.random.split(key)
    base = jnp.clip(jax.random.normal(key_base, (TOKENS, D), jnp.float32), -6.0, 6.0)
    chosen = jax.random.randint(key_block, (TOKENS, 1), 0, D // COLS_RA)
    column_block = jnp.arange(D, dtype=jnp.int32)[None, :] // COLS_RA
    boosted = jnp.where(column_block == chosen, 4.0, 1.0)
    return (base * boosted).astype(jnp.bfloat16)


def shard_levels(rng, shape, cuts, low, largest):
    level, own = 1.0, jax.random.fold_in(rng, 6)
    for axis_at, shards_of in cuts:
        draws = jnp.exp(jax.random.uniform(jax.random.fold_in(own, axis_at), (shards_of,), jnp.float32, low / len(cuts), largest / len(cuts)))
        level = level * jnp.repeat(draws, shape[axis_at] // shards_of).reshape([-1 if axis == axis_at else 1 for axis in range(len(shape))])
    return level


def normal_values(own_key, extent, width, most, shards=(), held_as=jnp.bfloat16):
    gain = shard_levels(own_key, extent, shards, -0.22, 0.18) if shards else 1.0
    result = jax.random.normal(own_key, extent, jnp.float32) * width * gain
    return jnp.minimum(jnp.maximum(result, -most), most).astype(held_as)


def setup_inputs(seed: int = 0) -> dict:
    arg_keys = jax.random.split(jax.random.key(seed), 8)
    return {
        "stream": draw_stream(jax.random.fold_in(arg_keys[7], 71), 0),
        "gain_first": jnp.clip(1.0 + 0.1 * jax.random.normal(arg_keys[1], (D,), jnp.float32), 0.5, 1.5),
        "up_first": normal_values(arg_keys[2], (D, FF), D ** -0.5, 0.1875, ((0, 8), (1, 4)), jnp.float32),
        "down_first": normal_values(arg_keys[3], (FF, D), FF ** -0.5, 0.09375, ((0, 4), (1, 8)), jnp.float32),
        "gain_second": jnp.clip(1.0 + 0.1 * jax.random.normal(arg_keys[4], (D,), jnp.float32), 0.5, 1.5),
        "up_second": normal_values(arg_keys[5], (D, FF), D ** -0.5, 0.1875, ((0, 8), (1, 4)), jnp.float32),
        "down_second": normal_values(arg_keys[6], (FF, D), FF ** -0.5, 0.09375, ((0, 4), (1, 8)), jnp.float32),
    }


EPS = 1e-06
RESIDUAL = 0.25

def sublayer(stream, norm_gain, w_up, w_down):
    floated = stream.astype(jnp.float32)
    squares = lax.optimization_barrier(jnp.sum(floated * floated, axis=1, keepdims=True))
    factor = jax.lax.rsqrt(squares / D + EPS)
    normed = (floated * factor * norm_gain.astype(jnp.float32)).astype(jnp.bfloat16)
    preact = jnp.dot(normed, w_up.astype(jnp.bfloat16), preferred_element_type=jnp.float32)
    activated = jnp.square(jax.nn.relu(preact)).astype(jnp.bfloat16)
    branch = jnp.dot(activated, w_down.astype(jnp.bfloat16), preferred_element_type=jnp.float32)
    return (RESIDUAL * floated + branch).astype(jnp.bfloat16)

def reference(stream, gain_first, up_first, down_first, gain_second, up_second, down_second):
    middle = sublayer(stream, gain_first, up_first, down_first)
    return sublayer(middle, gain_second, up_second, down_second)
```

```python
import functools

import jax
import jax.numpy as jnp
from jax import lax
from jax.experimental import pallas as pl
from jax.experimental.pallas import tpu as pltpu
from jax.sharding import PartitionSpec as P

EPS = 1e-06
RESIDUAL = 0.25
LANES = 128
ROWS = 8
MESH = pl.DeviceIdType.MESH
F32 = jnp.float32
BF16 = jnp.bfloat16


def kernel(
    n, m, width,
    stream_hbm, gain1_hbm, up1_hbm, down1_hbm, gain2_hbm, up2_hbm, down2_hbm,
    out_ref,
    stream_v, gain_v, up_v, down_v, down_b,
    part_out, part_in, sq_out, sq_in, act, branch_in,
    load_sem, part_ss, part_rs, sq_ss, sq_rs, act_ss, act_rs, br_ss, br_rs,
):
    ra = lax.axis_index("ra")
    cb = lax.axis_index("cb")
    tokens = stream_v.shape[0]
    block = part_out.shape[-1]

    def ra_peer(step):
        return lax.rem(ra + step, n)

    def cb_peer(step):
        return lax.rem(cb + step, m)

    loads = [
        pltpu.make_async_copy(src, dst, load_sem.at[i])
        for i, (src, dst) in enumerate((
            (stream_hbm, stream_v),
            (gain1_hbm, gain_v.at[0]),
            (up1_hbm, up_v.at[0]),
            (down1_hbm, down_v.at[0]),
            (gain2_hbm, gain_v.at[1]),
            (up2_hbm, up_v.at[1]),
            (down2_hbm, down_v.at[1]),
        ))
    ]
    barrier = pltpu.get_barrier_semaphore()
    for step in range(1, n):
        pl.semaphore_signal(barrier, inc=1, device_id={"ra": ra_peer(step)}, device_id_type=MESH)
    for step in range(1, m):
        pl.semaphore_signal(barrier, inc=1, device_id={"cb": cb_peer(step)}, device_id_type=MESH)
    for load in loads:
        load.start()

    def to_ra(src, dst, send, recv, peer):
        return pltpu.make_async_remote_copy(
            src_ref=src, dst_ref=dst, send_sem=send, recv_sem=recv,
            device_id={"ra": peer}, device_id_type=MESH,
        )

    def to_cb(src, dst, send, recv, peer):
        return pltpu.make_async_remote_copy(
            src_ref=src, dst_ref=dst, send_sem=send, recv_sem=recv,
            device_id={"cb": peer}, device_id_type=MESH,
        )

    sends = []
    for load in loads[:2]:
        load.wait()
    floated = stream_v[...].astype(F32)
    result = None
    for layer in range(2):
        scaled = (floated * gain_v[layer]).astype(BF16)
        loads[2 + 3 * layer].wait()
        partial = jnp.dot(scaled, up_v[layer].astype(BF16), preferred_element_type=F32)
        for j in range(n):
            part_out[layer, j] = partial[:, j * block:(j + 1) * block].astype(BF16)
        own = jnp.sum(floated * floated, axis=1, keepdims=True)
        sq_out[layer] = jnp.broadcast_to(own, (tokens, LANES)).T[:ROWS]
        if layer == 0:
            pl.semaphore_wait(barrier, n + m - 2)
        copies = []
        for step in range(1, n):
            peer = ra_peer(step)
            copies.append(to_ra(
                part_out.at[layer, peer], part_in.at[layer, ra],
                part_ss.at[layer, peer], part_rs.at[layer, ra], peer))
        for step in range(1, n):
            peer = ra_peer(step)
            copies.append(to_ra(
                sq_out.at[layer], sq_in.at[layer, ra],
                sq_ss.at[layer, peer], sq_rs.at[layer, ra], peer))
        for copy in copies:
            copy.start()
        sends += copies

        loads[3 + 3 * layer].wait()
        for j in range(n):
            down_b[layer, j] = down_v[layer, j * block:(j + 1) * block, :].astype(BF16)

        preact = part_out[layer, ra].astype(F32)
        for step in range(1, n):
            peer = ra_peer(step)
            to_ra(part_out.at[layer, peer], part_in.at[layer, peer],
                  part_ss.at[layer, peer], part_rs.at[layer, peer], peer).wait_recv()
            preact += part_in[layer, peer].astype(F32)
        positive = jnp.maximum(preact, 0.0)
        act[layer, ra] = (positive * positive).astype(BF16)

        copies = []
        for step in range(1, n):
            peer = ra_peer(step)
            copies.append(to_ra(
                act.at[layer, ra], act.at[layer, ra],
                act_ss.at[layer, peer], act_rs.at[layer, ra], peer))
        for copy in copies:
            copy.start()
        sends += copies

        squares = sq_out[layer]
        for step in range(1, n):
            peer = ra_peer(step)
            to_ra(sq_out.at[layer], sq_in.at[layer, peer],
                  sq_ss.at[layer, peer], sq_rs.at[layer, peer], peer).wait_recv()
            squares += sq_in[layer, peer]
        factor = 1.0 / (squares / width + EPS)
        scale = jnp.broadcast_to(factor[:1], (LANES, tokens)).T[:, :1]

        total = jnp.dot(act[layer, ra], down_b[layer, ra], preferred_element_type=F32)
        for step in range(1, n):
            peer = ra_peer(step)
            to_ra(act.at[layer, peer], act.at[layer, peer],
                  act_ss.at[layer, peer], act_rs.at[layer, peer], peer).wait_recv()
            total += jnp.dot(act[layer, peer], down_b[layer, peer], preferred_element_type=F32)

        branch_in[layer, cb] = (total * scale).astype(BF16)
        copies = []
        for step in range(1, m):
            peer = cb_peer(step)
            copies.append(to_cb(
                branch_in.at[layer, cb], branch_in.at[layer, cb],
                br_ss.at[layer, peer], br_rs.at[layer, cb], peer))
        for copy in copies:
            copy.start()
        sends += copies
        if layer == 0:
            loads[4].wait()
        for step in range(1, m):
            peer = cb_peer(step)
            to_cb(branch_in.at[layer, peer], branch_in.at[layer, peer],
                  br_ss.at[layer, peer], br_rs.at[layer, peer], peer).wait_recv()
        branch = branch_in[layer, 0].astype(F32)
        for j in range(1, m):
            branch += branch_in[layer, j].astype(F32)
        result = (RESIDUAL * floated + branch).astype(BF16)
        floated = result.astype(F32)
    out_ref[...] = result
    for copy in sends:
        copy.wait_send()


def local(n, m, stream, gain_first, up_first, down_first, gain_second, up_second, down_second):
    tokens, cols = stream.shape
    hidden = up_first.shape[1]
    block = hidden // n
    dma = pltpu.SemaphoreType.DMA
    return pl.pallas_call(
        functools.partial(kernel, n, m, cols * n),
        out_shape=jax.ShapeDtypeStruct((tokens, cols), BF16),
        in_specs=[pl.BlockSpec(memory_space=pl.ANY)] * 7,
        out_specs=pl.BlockSpec(memory_space=pltpu.VMEM),
        scratch_shapes=[
            pltpu.VMEM((tokens, cols), BF16),
            pltpu.VMEM((2, 1, cols), F32),
            pltpu.VMEM((2, cols, hidden), F32),
            pltpu.VMEM((2, hidden, cols), F32),
            pltpu.VMEM((2, n, block, cols), BF16),
            pltpu.VMEM((2, n, tokens, block), BF16),
            pltpu.VMEM((2, n, tokens, block), BF16),
            pltpu.VMEM((2, ROWS, tokens), F32),
            pltpu.VMEM((2, n, ROWS, tokens), F32),
            pltpu.VMEM((2, n, tokens, block), BF16),
            pltpu.VMEM((2, m, tokens, cols), BF16),
            dma((7,)),
            dma((2, n)), dma((2, n)),
            dma((2, n)), dma((2, n)),
            dma((2, n)), dma((2, n)),
            dma((2, m)), dma((2, m)),
        ],
        compiler_params=pltpu.CompilerParams(
            collective_id=0, has_side_effects=True
        ),
    )(
        stream, gain_first.reshape(1, cols), up_first, down_first,
        gain_second.reshape(1, cols), up_second, down_second,
    )


def solution(mesh):
    return jax.shard_map(
        functools.partial(local, mesh.shape["ra"], mesh.shape["cb"]),
        mesh=mesh,
        in_specs=(
            P(None, "ra"),
            P("ra"),
            P("ra", "cb"),
            P("cb", "ra"),
            P("ra"),
            P("ra", "cb"),
            P("cb", "ra"),
        ),
        out_specs=P(None, "ra"),
        check_vma=False,
    )
```

```python
import functools

import jax
import jax.numpy as jnp
from jax import lax
from jax.experimental import pallas as pl
from jax.experimental.pallas import tpu as pltpu
from jax.sharding import PartitionSpec as P

EPS = 1e-06
RESIDUAL = 0.25
LANES = 128
ROWS = 8
MESH = pl.DeviceIdType.MESH
F32 = jnp.float32
BF16 = jnp.bfloat16


def kernel(
    n, m, width,
    stream_hbm, gain1_hbm, up1_hbm, down1_hbm, gain2_hbm, up2_hbm, down2_hbm,
    out_ref,
    stream_v, gain_v, up_v, up_b, down_v, down_b,
    part_out, part_in, sq_out, sq_in, act, branch_in,
    load_sem, part_ss, part_rs, sq_ss, sq_rs, act_ss, act_rs, br_ss, br_rs,
):
    ra = lax.axis_index("ra")
    cb = lax.axis_index("cb")
    tokens = stream_v.shape[0]
    block = part_out.shape[-1]

    pair = 2 if n % 2 == 0 else 1
    half = lax.div(2 * ra, n)
    own_group = half * lax.div(ra, pair) + (1 - half) * (n // pair - 1 - lax.div(ra, pair))
    own_place = pair * own_group

    def ra_peer(step):
        place = step - 1
        place = place + lax.div(place - own_place + n, n)
        group = lax.div(place, pair)
        group = half * group + (1 - half) * (n // pair - 1 - group)
        return pair * group + lax.rem(ra + place, pair)

    def cb_peer(step):
        return lax.rem(cb + step, m)

    loads = [
        pltpu.make_async_copy(src, dst, load_sem.at[i])
        for i, (src, dst) in enumerate((
            (stream_hbm, stream_v),
            (gain1_hbm, gain_v.at[0]),
            (up1_hbm, up_v.at[0]),
            (down1_hbm, down_v.at[0]),
            (gain2_hbm, gain_v.at[1]),
            (up2_hbm, up_v.at[1]),
            (down2_hbm, down_v.at[1]),
        ))
    ]
    barrier = pltpu.get_barrier_semaphore()
    for step in range(1, n):
        pl.semaphore_signal(barrier, inc=1, device_id={"ra": ra_peer(step)}, device_id_type=MESH)
    for step in range(1, m):
        pl.semaphore_signal(barrier, inc=1, device_id={"cb": cb_peer(step)}, device_id_type=MESH)
    for load in loads:
        load.start()

    def to_ra(src, dst, send, recv, peer):
        return pltpu.make_async_remote_copy(
            src_ref=src, dst_ref=dst, send_sem=send, recv_sem=recv,
            device_id={"ra": peer}, device_id_type=MESH,
        )

    def to_cb(src, dst, send, recv, peer):
        return pltpu.make_async_remote_copy(
            src_ref=src, dst_ref=dst, send_sem=send, recv_sem=recv,
            device_id={"cb": peer}, device_id_type=MESH,
        )

    sends = []
    for load in loads[:2]:
        load.wait()
    floated = stream_v[...].astype(F32)
    result = None
    for layer in range(2):
        scaled = (floated * gain_v[layer]).astype(BF16)
        if layer == 0:
            loads[2].wait()
        up = up_v[layer].astype(BF16) if layer == 0 else up_b[...]
        partial = jnp.dot(scaled, up, preferred_element_type=F32)
        for j in range(n):
            part_out[layer, j] = partial[:, j * block:(j + 1) * block].astype(BF16)
        if layer == 0:
            pl.semaphore_wait(barrier, n + m - 2)
        copies = []
        for step in range(1, n):
            peer = ra_peer(step)
            copies.append(to_ra(
                part_out.at[layer, peer], part_in.at[layer, ra],
                part_ss.at[layer, peer], part_rs.at[layer, ra], peer))
        for copy in copies:
            copy.start()
        sends += copies
        own = jnp.sum(floated * floated, axis=1, keepdims=True)
        sq_out[layer] = jnp.broadcast_to(own, (tokens, LANES)).T[:ROWS]
        copies = []
        for step in range(1, n):
            peer = ra_peer(step)
            copies.append(to_ra(
                sq_out.at[layer], sq_in.at[layer, ra],
                sq_ss.at[layer, peer], sq_rs.at[layer, ra], peer))
        for copy in copies:
            copy.start()
        sends += copies

        loads[3 + 3 * layer].wait()
        for j in range(n):
            down_b[layer, j] = down_v[layer, j * block:(j + 1) * block, :].astype(BF16)

        preact = part_out[layer, ra].astype(F32)
        for step in range(1, n):
            peer = ra_peer(step)
            to_ra(part_out.at[layer, peer], part_in.at[layer, peer],
                  part_ss.at[layer, peer], part_rs.at[layer, peer], peer).wait_recv()
            preact += part_in[layer, peer].astype(F32)
        positive = jnp.maximum(preact, 0.0)
        act[layer, ra] = (positive * positive).astype(BF16)

        copies = []
        for step in range(1, n):
            peer = ra_peer(step)
            copies.append(to_ra(
                act.at[layer, ra], act.at[layer, ra],
                act_ss.at[layer, peer], act_rs.at[layer, ra], peer))
        for copy in copies:
            copy.start()
        sends += copies

        if layer == 0:
            loads[5].wait()
            up_b[...] = up_v[1].astype(BF16)

        squares = sq_out[layer]
        for step in range(1, n):
            peer = ra_peer(step)
            to_ra(sq_out.at[layer], sq_in.at[layer, peer],
                  sq_ss.at[layer, peer], sq_rs.at[layer, peer], peer).wait_recv()
            squares += sq_in[layer, peer]
        factor = 1.0 / (squares / width + EPS)
        scale = jnp.broadcast_to(factor[:1], (LANES, tokens)).T[:, :1]

        total = jnp.dot(act[layer, ra], down_b[layer, ra], preferred_element_type=F32)
        for step in range(1, n):
            peer = ra_peer(step)
            to_ra(act.at[layer, peer], act.at[layer, peer],
                  act_ss.at[layer, peer], act_rs.at[layer, peer], peer).wait_recv()
            total += jnp.dot(act[layer, peer], down_b[layer, peer], preferred_element_type=F32)

        branch_in[layer, cb] = (total * scale).astype(BF16)
        copies = []
        for step in range(1, m):
            peer = cb_peer(step)
            copies.append(to_cb(
                branch_in.at[layer, cb], branch_in.at[layer, cb],
                br_ss.at[layer, peer], br_rs.at[layer, cb], peer))
        for copy in copies:
            copy.start()
        sends += copies
        if layer == 0:
            loads[4].wait()
        for step in range(1, m):
            peer = cb_peer(step)
            to_cb(branch_in.at[layer, peer], branch_in.at[layer, peer],
                  br_ss.at[layer, peer], br_rs.at[layer, peer], peer).wait_recv()
        branch = branch_in[layer, 0].astype(F32)
        for j in range(1, m):
            branch += branch_in[layer, j].astype(F32)
        result = (RESIDUAL * floated + branch).astype(BF16)
        floated = result.astype(F32)
    out_ref[...] = result
    for copy in sends:
        copy.wait_send()


def local(n, m, stream, gain_first, up_first, down_first, gain_second, up_second, down_second):
    tokens, cols = stream.shape
    hidden = up_first.shape[1]
    block = hidden // n
    dma = pltpu.SemaphoreType.DMA
    return pl.pallas_call(
        functools.partial(kernel, n, m, cols * n),
        out_shape=jax.ShapeDtypeStruct((tokens, cols), BF16),
        in_specs=[pl.BlockSpec(memory_space=pl.ANY)] * 7,
        out_specs=pl.BlockSpec(memory_space=pltpu.VMEM),
        scratch_shapes=[
            pltpu.VMEM((tokens, cols), BF16),
            pltpu.VMEM((2, 1, cols), F32),
            pltpu.VMEM((2, cols, hidden), F32),
            pltpu.VMEM((cols, hidden), BF16),
            pltpu.VMEM((2, hidden, cols), F32),
            pltpu.VMEM((2, n, block, cols), BF16),
            pltpu.VMEM((2, n, tokens, block), BF16),
            pltpu.VMEM((2, n, tokens, block), BF16),
            pltpu.VMEM((2, ROWS, tokens), F32),
            pltpu.VMEM((2, n, ROWS, tokens), F32),
            pltpu.VMEM((2, n, tokens, block), BF16),
            pltpu.VMEM((2, m, tokens, cols), BF16),
            dma((7,)),
            dma((2, n)), dma((2, n)),
            dma((2, n)), dma((2, n)),
            dma((2, n)), dma((2, n)),
            dma((2, m)), dma((2, m)),
        ],
        compiler_params=pltpu.CompilerParams(
            collective_id=0, has_side_effects=True
        ),
    )(
        stream, gain_first.reshape(1, cols), up_first, down_first,
        gain_second.reshape(1, cols), up_second, down_second,
    )


def solution(mesh):
    return jax.shard_map(
        functools.partial(local, mesh.shape["ra"], mesh.shape["cb"]),
        mesh=mesh,
        in_specs=(
            P(None, "ra"),
            P("ra"),
            P("ra", "cb"),
            P("cb", "ra"),
            P("ra"),
            P("ra", "cb"),
            P("cb", "ra"),
        ),
        out_specs=P(None, "ra"),
        check_vma=False,
    )
```
